32 devices in a mesh: sp: 16 (over z, y, x), tp: 2 (over core).
Axes of the slice: x: 2, y: 2, z: 4, core: 2. Of those that a mesh axis runs over, the one named last changes fastest.
Arguments:
- conv_in: bfloat16 [4096, 1024], P('sp', 'tp'), may hold values from -6 to 6
- gate_outer: bfloat16 [4096, 1024], P('sp', 'tp'), may hold values from -6 to 6
- gate_inner: bfloat16 [4096, 1024], P('sp', 'tp'), may hold values from -6 to 6
- tap_weights: float32 [3, 1024], P(None, 'tp'), may hold values from -3 to 3
- doc_ids: int32 [4096], P('sp'), may hold values from 0 to 7, never falling along the last dimension, each value on 1 to 1024 neighbouring positions
- w_proj: bfloat16 [1024, 2048], replicated, may hold values from -0.1875 to 0.1875
- stream: bfloat16 [4096, 2048], P(('sp', 'tp')), may hold values from -6 to 6
- norm_gain: float32 [2048], replicated, may hold values from 0.1 to 1.9
- routes: int32 [4096, 4], P(('sp', 'tp')), may hold values from 0 to 31, all different within a row; in each aligned block of 128 rows (0 to 127, 128 to 255, ...) at most 32 rows name the same one
- route_weights: float32 [4096, 4], P(('sp', 'tp')), may hold values from 0.1 to 1
- w_gate: bfloat16 [32, 2048, 768], P(('sp', 'tp')), may hold values from -0.5 to 0.5
- w_up: bfloat16 [32, 2048, 768], P(('sp', 'tp')), may hold values from -0.5 to 0.5
- w_down: bfloat16 [32, 768, 2048], P(('sp', 'tp')), may hold values from -0.0546875 to 0.0546875
Outputs:
- layer_out: bfloat16 [4096, 2048], P(('sp', 'tp'))
The draws below stay inside these ranges and needn't reach their ends.
Inputs may be any that keep to these rules, and one draw needn't show every extreme that they name: `doc_ids`: document numbers never fall along the sequence; a document covers at most 1024 positions. `routes`: a token names 4 different experts; among the rows of one device (aligned blocks of 128 tokens) no expert is named more than 32 times, a bound that some block reaches.
All inputs are finite; a program needn't handle non-finite values.
Results may differ from the reference program's by a relative error of at most 0.0071.
Values may be sent and summed in bfloat16 or wider, within the bound.
A program may use at most 128 MiB of HBM per device.

```python
import math
import jax
import jax.numpy as jnp
import numpy as np
from jax import lax

D = 2048
CW = 1024
FF = 768
TOPK = 4
TAPS = 3
TOK_DEV = 256
TOKENS = 4096
EXPERTS = 32
BLOCK = 128
CAP = 32
DOCS = 8
DOC_MOST = 1024
N_TP = 2


def block_scale(own_key, dims, split, low, top_value):
    def one(position, blocks):
        draws = jax.random.uniform(jax.random.fold_in(jax.random.fold_in(own_key, 6), position), (blocks,), jnp.float32, low / len(split), top_value / len(split))
        return jnp.repeat(jnp.exp(draws), dims[position] // blocks).reshape((-1,) + (1,) * (len(dims) - position - 1))

    factor_of = one(*split[0])
    for cut in split[1:]:
        factor_of = factor_of * one(*cut)
    return factor_of


def split_up(number_of, total, most, skew):
    portions = [(1 << 20) // math.isqrt(rank ** skew) + 1 for rank in range(2, number_of + 1)]
    rest, holding = total - most - (number_of - 1), [1] * (number_of - 1)
    while rest > 0:
        movable = [i for i in range(number_of - 1) if holding[i] < most]
        whole, remaining = sum([portions[i] for i in movable]), rest
        for i in movable:
            extra = min(most - holding[i], max(1, remaining * portions[i] // whole), rest)
            holding[i] = holding[i] + extra
            rest = rest - extra
    return np.array([most] + holding)


def ragged(own_key, count, total, bound, lean):
    if count == 2:
        one = jax.random.randint(own_key, (), max(1, total - bound), min(bound, total - 1) + 1)
        return jnp.stack([one, total - one])
    sizes = jnp.asarray(split_up(count, total, bound, lean), jnp.int32)
    twos = (count - 1) // 2
    giver, taker = sizes[1:1 + 2 * twos:2], sizes[2:2 + 2 * twos:2]
    margin = jnp.minimum(giver - 1, bound - taker)
    passed = jax.random.randint(jax.random.fold_in(own_key, 1), (twos,), 0, 1 << 20) % (margin + 1)
    sizes = sizes.at[1:1 + 2 * twos:2].set(giver - passed).at[2:2 + 2 * twos:2].set(taker + passed)
    return sizes[jax.random.permutation(jax.random.fold_in(own_key, 2), count)]


def shared_out(own_key, own, number, rows, amount, top, most, slope):
    ranking = jax.random.permutation(own_key, amount)
    heavy_load, common = portions_of(amount, rows * top, most, slope, True), portions_of(amount, rows * top, most, slope, False)
    places = jnp.arange(amount)

    def named(lengths, offset_by):
        used = int((lengths > 0).sum())
        fixed = max(1, used // 4)
        moved = fixed + (places - fixed + offset_by * (used - fixed)) % max(1, amount - fixed)
        return jnp.zeros((amount,), jnp.int32).at[ranking[jnp.where(places < fixed, places, moved)]].set(jnp.asarray(lengths, jnp.int32))

    lengths = jnp.where(number % 4 == 0, named(heavy_load, number // 4), named(common, number - number // 4 - 1))
    mixed = jax.random.permutation(jax.random.fold_in(own, 3), amount)
    donor, sink = mixed[0:amount // 2 * 2:2], mixed[1:amount // 2 * 2:2]
    room = jnp.minimum(lengths[donor] - 1, most - lengths[sink]) // 2
    room = jnp.where((donor == ranking[0]) | (sink == ranking[0]) | (lengths[sink] == 0), 0, jnp.maximum(room, 0))
    moved = jax.random.randint(jax.random.fold_in(own, 4), (amount // 2,), 0, 1 << 20) % (room + 1)
    lengths = lengths.at[donor].add(-moved).at[sink].add(moved)
    members = jnp.searchsorted(jnp.cumsum(lengths), jnp.arange(rows * top), side="right").astype(jnp.int32)
    table = members.reshape(top, rows).T
    table = table[jax.random.permutation(jax.random.fold_in(own, 1), rows)]
    offset_by = jax.random.randint(jax.random.fold_in(own, 2), (rows, 1), 0, top)
    return jnp.take_along_axis(table, (jnp.arange(top)[None, :] + offset_by) % top, axis=1)


def portions_of(amount, total, most, skew, full):
    portions = [(1 << 20) // math.isqrt(grade ** skew) + 1 for grade in range(1, amount + 1)]
    largest = most if full else min(most, max(-(-total // amount), total * portions[0] // sum(portions)))
    least = 1 if total - largest >= amount - 1 else 0
    holding, rest = [largest] + [least] * (amount - 1), total - largest - least * (amount - 1)
    while rest > 0:
        free = [i for i in range(1, amount) if holding[i] < largest] or [i for i in range(1, amount) if holding[i] < most]
        pool, remaining = sum([portions[i] for i in free]), rest
        for i in free:
            more = min(most - holding[i], max(1, remaining * portions[i] // pool), rest)
            holding[i] = holding[i] + more
            rest = rest - more
    return np.array(holding)


def noise(rng, shape, width, limit, pieces=(), held_as=jnp.bfloat16):
    entries = width * jax.random.normal(rng, shape, jnp.float32)
    if pieces:
        entries = entries * block_scale(rng, shape, pieces, -0.22, 0.18)
    return jnp.clip(entries, -limit, limit).astype(held_as)


def setup_inputs(seed: int = 0) -> dict:
    arg_keys = jax.random.split(jax.random.key(seed), 14)
    conv_in = noise(arg_keys[0], (TOKENS, CW), 1.0, 6.0, ((0, 16), (1, 2)))
    gate_outer = noise(arg_keys[1], (TOKENS, CW), 1.0, 6.0, ((0, 16), (1, 2)))
    gate_inner = noise(arg_keys[2], (TOKENS, CW), 1.0, 6.0, ((0, 16), (1, 2)))
    tap_weights = noise(arg_keys[3], (TAPS, CW), 0.6, 3.0, ((1, 2),), jnp.float32)
    doc_ids = jnp.searchsorted(jnp.cumsum(ragged(arg_keys[4], DOCS, TOKENS, DOC_MOST, 0)), jnp.arange(TOKENS), side="right").astype(jnp.int32)
    w_proj = noise(arg_keys[5], (CW, D), CW ** -0.5, 0.1875)
    stream = noise(arg_keys[6], (TOKENS, D), 1.0, 6.0, ((0, 32),))
    norm_gain = jnp.clip(1.0 + 0.18 * jax.random.normal(arg_keys[7], (D,), jnp.float32), 0.1, 1.9)
    routes_keys = jax.random.split(jax.random.fold_in(arg_keys[8], 1), TOKENS // BLOCK)
    routes_turns = jax.random.permutation(jax.random.fold_in(arg_keys[8], 3), TOKENS // BLOCK)
    routes = jax.vmap(lambda own, number: shared_out(jax.random.fold_in(arg_keys[8], 2), own, number, BLOCK, EXPERTS, TOPK, CAP, 1))(routes_keys, routes_turns).reshape((TOKENS, TOPK))
    route_weights = jnp.clip(jnp.exp(math.log(1.0) - 2.3025851 * jax.random.uniform(arg_keys[9], (TOKENS, TOPK), jnp.float32) ** block_scale(arg_keys[9], (TOKENS, TOPK), ((0, 32),), -0.2, 0.2)), 0.1, 1.0)
    w_gate = noise(arg_keys[10], (EXPERTS, D, FF), (D // 16) ** -0.5, 0.5, ((0, 32),))
    w_up = noise(arg_keys[11], (EXPERTS, D, FF), (D // 16) ** -0.5, 0.5, ((0, 32),))
    w_down = noise(arg_keys[12], (EXPERTS, FF, D), (16 * FF) ** -0.5, 0.0546875, ((0, 32),))
    return dict(conv_in=conv_in, gate_outer=gate_outer, gate_inner=gate_inner, tap_weights=tap_weights, doc_ids=doc_ids, w_proj=w_proj, stream=stream, norm_gain=norm_gain, routes=routes, route_weights=route_weights, w_gate=w_gate, w_up=w_up, w_down=w_down)


def expert_rows(rows, wg, wu, wd):
    gate = jnp.minimum(jnp.dot(rows, wg, preferred_element_type=jnp.float32), 7.0)
    upper = jnp.clip(jnp.dot(rows, wu, preferred_element_type=jnp.float32), -7.0, 7.0)
    act = ((upper + 1.0) * gate * jax.nn.sigmoid(1.702 * gate)).astype(jnp.bfloat16)
    return jnp.dot(act, wd, preferred_element_type=jnp.float32).astype(jnp.bfloat16)

def reference(conv_in, gate_outer, gate_inner, tap_weights, doc_ids, w_proj, stream, norm_gain, routes, route_weights, w_gate, w_up, w_down):
    product = gate_inner.astype(jnp.float32) * conv_in.astype(jnp.float32)
    same = (doc_ids[1:] == doc_ids[:-1]).astype(jnp.float32)
    zero_row = jnp.zeros((1, product.shape[1]), jnp.float32)
    before = jnp.concatenate([zero_row, product[:-1] * same[:, None]], axis=0)
    after = jnp.concatenate([product[1:] * same[:, None], zero_row], axis=0)
    conv = tap_weights[0] * before + tap_weights[1] * product + tap_weights[2] * after
    mixed = (gate_outer.astype(jnp.float32) * conv).astype(jnp.bfloat16)
    hidden = stream.astype(jnp.float32) + jnp.dot(mixed, w_proj, preferred_element_type=jnp.float32)
    scale = lax.rsqrt(lax.optimization_barrier(jnp.mean(hidden * hidden, axis=-1, keepdims=True)) + 1e-05)
    normed = (hidden * scale * norm_gain).astype(jnp.bfloat16)
    block = TOK_DEV // N_TP
    nblocks = TOKENS // block
    slots = nblocks * CAP
    chosen = routes.reshape(nblocks, block * TOPK)
    onehot = (chosen[:, :, None] == jnp.arange(EXPERTS, dtype=jnp.int32)[None, None, :]).astype(jnp.int32)
    ranks = lax.optimization_barrier(jnp.sum(jnp.cumsum(onehot, axis=1) * onehot, axis=-1)) - 1
    block_ids = jnp.arange(nblocks, dtype=jnp.int32)[:, None]
    places = (chosen * slots + block_ids * CAP + ranks).reshape(-1).astype(jnp.int32)
    owners = (block_ids * block + (jnp.arange(block * TOPK, dtype=jnp.int32) // TOPK)[None, :]).reshape(-1)
    table = jnp.full((EXPERTS * slots,), TOKENS, jnp.int32).at[places].set(owners).reshape(EXPERTS, slots)
    weights = jnp.zeros((EXPERTS * slots,), jnp.float32).at[places].set(route_weights.reshape(-1)).reshape(EXPERTS, slots)
    padded = jnp.concatenate([normed, jnp.zeros((1, normed.shape[1]), jnp.bfloat16)], axis=0)

    def one_expert(total, items):
        owner_ids, owner_weights, wg, wu, wd = items
        result = expert_rows(padded[owner_ids], wg, wu, wd)
        total = total.at[owner_ids].add(result.astype(jnp.float32) * owner_weights[:, None])
        return (total, None)
    start = jnp.zeros((TOKENS + 1, normed.shape[1]), jnp.float32)
    total, _ = lax.scan(one_expert, start, (table, weights, w_gate, w_up, w_down))
    return (hidden + total[:TOKENS]).astype(jnp.bfloat16)
```

```python
import functools
import math

import jax
import jax.numpy as jnp
from jax import lax
from jax.experimental import pallas as pl
from jax.experimental.pallas import tpu as pltpu
from jax.sharding import PartitionSpec as P

MESH = pl.DeviceIdType.MESH


def with_halo(shard, sides, width):
    for axis, dim in sides:
        size, length = (lax.axis_size(axis), shard.shape[dim])
        up = [(i, (i + 1) % size) for i in range(size - 1)]
        down = [(j, i) for i, j in up]
        last = lax.slice_in_dim(shard, length - width, length, axis=dim)
        initial = lax.slice_in_dim(shard, 0, width, axis=dim)
        before = lax.ppermute(last, axis, up)
        after = lax.ppermute(initial, axis, down)
        shard = jnp.concatenate([before, shard, after], axis=dim)
    return shard


def dot(a, b):
    return jnp.dot(a, b, preferred_element_type=jnp.float32)


def tile_of(size, most):
    return next(t for t in range(most, 0, -128) if size % t == 0)


def schedule(steps):
    order, d, f, c = [], 0, 0, 0
    while c < steps:
        while d < steps and d < f + 2:
            order.append(("d", d))
            d += 1
        if f < steps:
            order.append(("f", f))
            f += 1
        if f - c >= 2 or f == steps:
            order.append(("c", c))
            c += 1
    return order


def moe_kernel(
    nz, n_plane, n_core, cap,
    normed, hidden, select, spread, wg_hbm, wu_hbm, wd_hbm,
    out_ref,
    wg, wu, wd, zbuf, outgoing, arrived, act, results, returned, partial, summed,
    w_sem, z_send, z_recv, a_send, a_recv, r_send, r_recv, p_send, p_recv,
):
    peers = n_plane * n_core
    width = normed.shape[1]
    rows = peers * cap
    ff = wg.shape[1]
    me = lax.axis_index("sp")
    core = lax.axis_index("tp")
    z, p = me // n_plane, lax.rem(me, n_plane)
    rank = p * n_core + core

    def z_peer(k):
        return {"sp": lax.rem(z + k, nz) * n_plane + p, "tp": core}

    def plane_peer(j):
        q = lax.rem(rank + j, peers)
        return {"sp": z * n_plane + q // n_core, "tp": lax.rem(q, n_core)}

    loads = [
        pltpu.make_async_copy(src, dst, w_sem.at[i])
        for i, (src, dst) in enumerate(((wg_hbm, wg), (wu_hbm, wu), (wd_hbm, wd)))
    ]
    for load in loads:
        load.start()
    barrier = pltpu.get_barrier_semaphore()
    for k in range(1, nz):
        pl.semaphore_signal(barrier, inc=1, device_id=z_peer(k), device_id_type=MESH)
    for j in range(1, peers):
        pl.semaphore_signal(barrier, inc=1, device_id=plane_peer(j), device_id_type=MESH)
    pl.semaphore_wait(barrier, nz - 1 + peers - 1)

    def remote(src, dst, send, recv, to):
        return pltpu.make_async_remote_copy(
            src_ref=src, dst_ref=dst, send_sem=send, recv_sem=recv,
            device_id=to, device_id_type=MESH)

    z_copies = {}
    for k in range(1, nz):
        z_copies[k] = remote(normed, zbuf.at[k - 1], z_send.at[k], z_recv.at[k], z_peer(k))
        z_copies[k].start()

    a_copies, r_copies, p_copies = {}, {}, {}
    col = tile_of(width, 512)
    fcol = tile_of(ff, 256)

    def dispatch(k):
        if k:
            z_copies[k].wait_recv()
        block = normed if k == 0 else zbuf.at[k - 1]

        @pl.loop(0, width // col)
        def _(i):
            cols = pl.ds(pl.multiple_of(i * col, col), col)
            picked = dot(select[k], block[:, cols]).astype(jnp.bfloat16)
            arrived[k, 0:cap, cols] = picked[:cap]
            outgoing[k, :, cols] = picked[cap:]

        for j in range(1, peers):
            a_copies[k, j] = remote(
                outgoing.at[k, pl.ds((j - 1) * cap, cap)], arrived.at[k, pl.ds(j * cap, cap)],
                a_send.at[k, j], a_recv.at[k, j], plane_peer(j))
            a_copies[k, j].start()

    def expert(k):
        if k == 0:
            for load in loads:
                load.wait()
        for j in range(1, peers):
            a_copies[k, j].wait_recv()

        @pl.loop(0, ff // fcol)
        def _(i):
            cols = pl.ds(pl.multiple_of(i * fcol, fcol), fcol)
            gate = jnp.minimum(dot(arrived[k], wg[:, cols]), 7.0)
            upper = jnp.clip(dot(arrived[k], wu[:, cols]), -7.0, 7.0)
            act[:, cols] = ((upper + 1.0) * gate * jax.nn.sigmoid(1.702 * gate)).astype(jnp.bfloat16)

        @pl.loop(0, width // col)
        def _(i):
            cols = pl.ds(pl.multiple_of(i * col, col), col)
            res = dot(act[...], wd[:, cols]).astype(jnp.bfloat16)
            returned[k, 0:cap, cols] = res[:cap]
            results[k, :, cols] = res[cap:]

        for j in range(1, peers):
            r_copies[k, j] = remote(
                results.at[k, pl.ds((j - 1) * cap, cap)], returned.at[k, pl.ds(j * cap, cap)],
                r_send.at[k, j], r_recv.at[k, j], plane_peer(peers - j))
            r_copies[k, j].start()

    def combine(k):
        for j in range(1, peers):
            r_copies[k, j].wait_recv()

        @pl.loop(0, width // col)
        def _(i):
            cols = pl.ds(pl.multiple_of(i * col, col), col)
            total = dot(spread[k], returned[k, :, cols])
            if k == 0:
                hidden[:, cols] = hidden[:, cols] + total
            else:
                partial[k - 1, :, cols] = total.astype(jnp.bfloat16)

        if k:
            p_copies[k] = remote(
                partial.at[k - 1], summed.at[k - 1], p_send.at[k], p_recv.at[k], z_peer(nz - k))
            p_copies[k].start()

    for kind, k in schedule(nz):
        {"d": dispatch, "f": expert, "c": combine}[kind](k)

    for k in range(1, nz):
        p_copies[k].wait_recv()

    @pl.loop(0, width // col)
    def _(i):
        cols = pl.ds(pl.multiple_of(i * col, col), col)
        total = hidden[:, cols]
        for k in range(1, nz):
            total = total + summed[k - 1, :, cols].astype(jnp.float32)
        out_ref[:, cols] = total.astype(jnp.bfloat16)

    for k in range(1, nz):
        z_copies[k].wait_send()
        p_copies[k].wait_send()
    for k in range(nz):
        for j in range(1, peers):
            a_copies[k, j].wait_send()
            r_copies[k, j].wait_send()


def moe(nz, n_plane, n_core, cap, normed, hidden, select, spread, wg, wu, wd):
    block, width = normed.shape
    ff = wg.shape[1]
    peers = n_plane * n_core
    rows = peers * cap
    bf = jnp.bfloat16
    vmem = pl.BlockSpec(memory_space=pltpu.VMEM)
    hbm = pl.BlockSpec(memory_space=pl.ANY)
    dma = pltpu.SemaphoreType.DMA

    def body(normed, hidden_in, *rest):
        hidden = rest[-1]
        hidden[...] = hidden_in[...]
        moe_kernel(nz, n_plane, n_core, cap, normed, hidden, *rest[:-1])

    return pl.pallas_call(
        body,
        out_shape=jax.ShapeDtypeStruct((block, width), bf),
        in_specs=[vmem] * 4 + [hbm] * 3,
        out_specs=vmem,
        scratch_shapes=[
            pltpu.VMEM((width, ff), bf),
            pltpu.VMEM((width, ff), bf),
            pltpu.VMEM((ff, width), bf),
            pltpu.VMEM((nz - 1, block, width), bf),
            pltpu.VMEM((nz, rows - cap, width), bf),
            pltpu.VMEM((nz, rows, width), bf),
            pltpu.VMEM((rows, ff), bf),
            pltpu.VMEM((nz, rows - cap, width), bf),
            pltpu.VMEM((nz, rows, width), bf),
            pltpu.VMEM((nz - 1, block, width), bf),
            pltpu.VMEM((nz - 1, block, width), bf),
            dma((3,)), dma((nz,)), dma((nz,)),
            dma((nz, peers)), dma((nz, peers)), dma((nz, peers)), dma((nz, peers)),
            dma((nz,)), dma((nz,)),
            pltpu.VMEM((block, width), jnp.float32),
        ],
        compiler_params=pltpu.CompilerParams(
            collective_id=0, has_side_effects=True, vmem_limit_bytes=60 * 2**20),
        name="moe_exchange",
    )(normed, hidden, select, spread, wg, wu, wd)


def slot_matrices(nz, n_plane, n_core, cap, routes, route_weights):
    block, topk = routes.shape
    peers = n_plane * n_core
    me = lax.axis_index("sp")
    z, p = me // n_plane, lax.rem(me, n_plane)
    rank = p * n_core + lax.axis_index("tp")
    groups = [[a * n_plane + b for a in range(nz)] for b in range(n_plane)]
    packed = jnp.concatenate([routes.astype(jnp.float32), route_weights], axis=1)
    every = lax.all_gather(packed, "sp", axis_index_groups=groups)
    every = every[(z - jnp.arange(nz)) % nz]
    chosen, weight = every[..., :topk].astype(jnp.int32), every[..., topk:]
    experts = z * peers + (rank + jnp.arange(peers)) % peers
    hit = chosen[..., None] == experts
    named = jnp.any(hit, axis=2)
    share = jnp.sum(jnp.where(hit, weight[..., None], 0.0), axis=2)
    below = jnp.tril(jnp.ones((block, block), jnp.bfloat16), -1)
    slot = jnp.einsum("ts,kse->kte", below, named.astype(jnp.bfloat16), preferred_element_type=jnp.float32)
    slot = jnp.where(named, slot.astype(jnp.int32), -1)
    place = slot[..., None] == jnp.arange(cap, dtype=jnp.int32)
    spread = jnp.where(place, share[..., None], 0.0).astype(jnp.bfloat16).reshape(nz, block, peers * cap)
    slot_t = jnp.swapaxes(slot, 1, 2)
    select = (slot_t[:, :, None, :] == jnp.arange(cap, dtype=jnp.int32)[:, None]).astype(jnp.bfloat16)
    return select.reshape(nz, peers * cap, block), spread


def per_device(
    conv_in,
    gate_outer,
    gate_inner,
    tap_weights,
    doc_ids,
    w_proj,
    stream,
    norm_gain,
    routes,
    route_weights,
    w_gate,
    w_up,
    w_down,
):
    n_seq = lax.axis_size("sp")
    n_core = lax.axis_size("tp")
    tok_dev = conv_in.shape[0]
    topk = routes.shape[1]
    n_expert = n_seq * n_core
    capacity = max(2, 2 * tok_dev * topk // (n_core * n_expert))
    capacity = -(-capacity // 16) * 16
    nz = max(d for d in range(1, math.isqrt(n_seq) + 1) if n_seq % d == 0)
    n_plane = n_seq // nz
    select, spread = slot_matrices(nz, n_plane, n_core, capacity, routes, route_weights)
    product = gate_inner.astype(jnp.float32) * conv_in.astype(jnp.float32)
    doc_float = doc_ids.astype(jnp.float32)
    wide_prod, wide_docs = (
        with_halo(product, (("sp", 0),), 1),
        with_halo(doc_float, (("sp", 0),), 1),
    )
    same_before = (wide_docs[1:-1] == wide_docs[:-2]).astype(jnp.float32)
    same_after = (wide_docs[1:-1] == wide_docs[2:]).astype(jnp.float32)
    conv = (
        tap_weights[0] * wide_prod[:-2] * same_before[:, None]
        + tap_weights[1] * product
        + tap_weights[2] * wide_prod[2:] * same_after[:, None]
    )
    mixed = (gate_outer.astype(jnp.float32) * conv).astype(jnp.bfloat16)
    regrouped = lax.all_to_all(mixed, "tp", split_axis=0, concat_axis=1, tiled=True)
    projected = jnp.dot(regrouped, w_proj, preferred_element_type=jnp.float32)
    hidden = stream.astype(jnp.float32) + projected
    scale = lax.rsqrt(jnp.mean(hidden * hidden, axis=-1, keepdims=True) + 1e-05)
    normed = (hidden * scale * norm_gain).astype(jnp.bfloat16)
    return moe(nz, n_plane, n_core, capacity, normed, hidden, select, spread, w_gate[0], w_up[0], w_down[0])


def solution(mesh):
    in_specs = (
        P("sp", "tp"),
        P("sp", "tp"),
        P("sp", "tp"),
        P(None, "tp"),
        P("sp"),
        P(),
        P(("sp", "tp"), None),
        P(),
        P(("sp", "tp"), None),
        P(("sp", "tp"), None),
        P(("sp", "tp"), None, None),
        P(("sp", "tp"), None, None),
        P(("sp", "tp"), None, None),
    )
    out_specs = P(("sp", "tp"), None)
    return jax.shard_map(
        per_device, mesh=mesh, in_specs=in_specs, out_specs=out_specs, check_vma=False
    )
```
